32 devices in a mesh: sp: 8 (over z, y), tp: 4 (over x, core).
Axes of the slice: x: 2, y: 2, z: 4, core: 2. Of those that a mesh axis runs over, the one named last changes fastest.
Arguments:
- tokens: bfloat16 [2048, 2048], P('sp'), may hold values from -6 to 6
- input_norm_gain: float32 [2048], replicated, may hold values from 0.1 to 1.9
- convolution_value_weight: bfloat16 [2048, 512], P(None, 'tp'), may hold values from -0.125 to 0.125
- convolution_gate_weight: bfloat16 [2048, 512], P(None, 'tp'), may hold values from -0.125 to 0.125
- depthwise_taps_weight: float32 [31, 512], P(None, 'tp'), may hold values from -1 to 1
- convolution_group_gain: float32 [512], P('tp'), may hold values from 0.1 to 1.9
- convolution_group_shift: float32 [512], P('tp'), may hold values from -3 to 3
- receptance_weight: bfloat16 [2048, 1024], P(None, 'tp'), may hold values from -0.125 to 0.125
- key_weight: bfloat16 [2048, 1024], P(None, 'tp'), may hold values from -0.125 to 0.125
- value_weight: bfloat16 [2048, 1024], P(None, 'tp'), may hold values from -0.125 to 0.125
- decay_weight: bfloat16 [2048, 1024], P(None, 'tp'), may hold values from -0.0625 to 0.0625
- correction_rate_weight: bfloat16 [2048, 1024], P(None, 'tp'), may hold values from -0.125 to 0.125
- output_gate_weight: bfloat16 [2048, 1024], P(None, 'tp'), may hold values from -0.125 to 0.125
- key_prenorm_gain: float32 [1024], P('tp'), may hold values from 0.04 to 8
- decay_offset_bias: float32 [1024], P('tp'), may hold values from -30 to 0
- position_decay_shift: float32 [2048, 1024], P('sp', 'tp'), may hold values from -1 to 1
- extra_log_decay: float32 [2048, 1024], P('sp', 'tp'), may hold values from -0.7 to 0
- head_norm_gain: float32 [1024], P('tp'), may hold values from 0.1 to 1.9
- convolution_output_weight: bfloat16 [512, 2048], replicated, may hold values from -0.15625 to 0.15625
- attention_output_weight: bfloat16 [1024, 2048], replicated, may hold values from -0.15625 to 0.15625
Outputs:
- mixed: bfloat16 [2048, 2048], P(('sp', 'tp'))
The draws below stay inside these ranges and needn't reach their ends.
All inputs are finite; a program needn't handle non-finite values.
Results may differ from the reference program's by a relative error of at most 0.0063.
The reference program's roundings to bfloat16 on the way (of `normed`, `conv_input`, `conv_out` and `mix_out`) count: a program that leaves them out, or rounds other values in their place, can miss the bound.
Values may be sent and summed in bfloat16 or wider, within the bound.
A program may use at most 128 MiB of HBM per device.

```python
import jax
import jax.numpy as jnp
from jax import lax

D = 2048
CONV_CH = 512
CONV_TAPS = 31
HEADS = 16
HEAD = 64
TOKENS = 2048
MIX_CH = 1024


def draw_key_prenorm_gain(key, part):
    second = jax.random.fold_in(jax.random.fold_in(key, 53), 1)
    gain = jnp.exp(jnp.log(0.04) + jnp.log(200.0) * jax.random.uniform(second, (HEADS * HEAD,)))
    return jnp.clip(gain, 0.04, 8.0).astype(jnp.float32)


def draw_decay_offset_bias(key, part):
    first, second, third, fourth = jax.random.split(jax.random.fold_in(key, 11), 4)
    share = 0.5
    slow_head = jax.random.uniform(first, (HEADS,)) < share
    keep_scale = jnp.exp(jnp.log(0.1) + jnp.log(6.0) * jax.random.uniform(second, (HEADS,)))
    fast_length = jax.random.uniform(third, (HEADS,), minval=25.0, maxval=50.0)
    level = jnp.where(slow_head, jnp.log(keep_scale / TOKENS), -jnp.log(fast_length)) + 0.5
    jitter = jnp.clip(0.3 * jax.random.normal(fourth, (HEADS, HEAD)), -1.0, 1.0)
    return (level[:, None] + jitter).reshape(HEADS * HEAD).astype(jnp.float32)


def draw_position_decay_shift(key, part):
    level_key = jax.random.fold_in(key, 23)
    block_count = (TOKENS + 127) // 128
    level = jax.random.uniform(level_key, (block_count, HEADS), minval=-0.7, maxval=0.7)
    spread_rows = jnp.repeat(level, 128, axis=0)[:TOKENS]
    return jnp.repeat(spread_rows, HEAD, axis=1).astype(jnp.float32)


def draw_extra_log_decay(key, part):
    first, second = jax.random.split(jax.random.fold_in(key, 37), 2)
    places = jax.random.randint(first, (6,), 0, TOKENS)
    kept = jax.random.uniform(second, (6, HEADS * HEAD), minval=0.5, maxval=0.8)
    return jnp.zeros((TOKENS, HEADS * HEAD), jnp.float32).at[places].min(jnp.log(kept))


def level_of(stream_key, dims, pieces, smallest, top_value):
    def one(dim, shards_of):
        draws = jax.random.uniform(jax.random.fold_in(jax.random.fold_in(stream_key, 6), dim), (shards_of,), jnp.float32, smallest / len(pieces), top_value / len(pieces))
        return jnp.repeat(jnp.exp(draws), dims[dim] // shards_of).reshape((-1,) + (1,) * (len(dims) - dim - 1))

    factor_of = one(*pieces[0])
    for cut in pieces[1:]:
        factor_of = factor_of * one(*cut)
    return factor_of


def normal_values(rng, extent, spread, limit, cuts=(), kind=jnp.bfloat16):
    entries = spread * jax.random.normal(rng, extent, jnp.float32)
    if cuts:
        entries = entries * level_of(rng, extent, cuts, -0.22, 0.18)
    return jnp.clip(entries, -limit, limit).astype(kind)


def setup_inputs(seed: int = 0) -> dict:
    splits = jax.random.split(jax.random.key(seed), 21)
    tokens = normal_values(splits[0], (TOKENS, D), 1.0, 6.0, ((0, 8),))
    input_norm_gain = jnp.clip(1.0 + 0.18 * jax.random.normal(splits[1], (D,), jnp.float32), 0.1, 1.9)
    convolution_value_weight = normal_values(splits[2], (D, CONV_CH), D ** -0.5, 0.125, ((1, 4),))
    convolution_gate_weight = normal_values(splits[3], (D, CONV_CH), D ** -0.5, 0.125, ((1, 4),))
    depthwise_taps_weight = normal_values(splits[4], (CONV_TAPS, CONV_CH), CONV_TAPS ** -0.5, 1.0, ((1, 4),), jnp.float32)
    convolution_group_gain = jnp.clip(1.0 + 0.18 * jax.random.normal(splits[5], (CONV_CH,), jnp.float32), 0.1, 1.9)
    convolution_group_shift = normal_values(splits[6], (CONV_CH,), 0.5, 3.0, ((0, 4),), jnp.float32)
    receptance_weight = normal_values(splits[7], (D, MIX_CH), D ** -0.5, 0.125, ((1, 4),))
    key_weight = normal_values(splits[8], (D, MIX_CH), D ** -0.5, 0.125, ((1, 4),))
    value_weight = normal_values(splits[9], (D, MIX_CH), D ** -0.5, 0.125, ((1, 4),))
    decay_weight = normal_values(splits[10], (D, MIX_CH), (4 * D) ** -0.5, 0.0625, ((1, 4),))
    correction_rate_weight = normal_values(splits[11], (D, MIX_CH), D ** -0.5, 0.125, ((1, 4),))
    output_gate_weight = normal_values(splits[12], (D, MIX_CH), D ** -0.5, 0.125, ((1, 4),))
    key_prenorm_gain = draw_key_prenorm_gain(jax.random.fold_in(splits[20], 71), 0)
    decay_offset_bias = draw_decay_offset_bias(jax.random.fold_in(splits[20], 71), 0)
    position_decay_shift = draw_position_decay_shift(jax.random.fold_in(splits[20], 71), 0)
    extra_log_decay = draw_extra_log_decay(jax.random.fold_in(splits[20], 71), 0)
    head_norm_gain = jnp.clip(1.0 + 0.18 * jax.random.normal(splits[17], (MIX_CH,), jnp.float32), 0.1, 1.9)
    convolution_output_weight = normal_values(splits[18], (CONV_CH, D), (CONV_CH + MIX_CH) ** -0.5, 0.15625)
    attention_output_weight = normal_values(splits[19], (MIX_CH, D), (CONV_CH + MIX_CH) ** -0.5, 0.15625)
    return dict(tokens=tokens, input_norm_gain=input_norm_gain, convolution_value_weight=convolution_value_weight, convolution_gate_weight=convolution_gate_weight, depthwise_taps_weight=depthwise_taps_weight, convolution_group_gain=convolution_group_gain, convolution_group_shift=convolution_group_shift, receptance_weight=receptance_weight, key_weight=key_weight, value_weight=value_weight, decay_weight=decay_weight, correction_rate_weight=correction_rate_weight, output_gate_weight=output_gate_weight, key_prenorm_gain=key_prenorm_gain, decay_offset_bias=decay_offset_bias, position_decay_shift=position_decay_shift, extra_log_decay=extra_log_decay, head_norm_gain=head_norm_gain, convolution_output_weight=convolution_output_weight, attention_output_weight=attention_output_weight)


NORM_EPS = 1e-06
GROUP_EPS = 1e-05
HEAD_EPS = 0.00064
KEY_EPS = 1e-06

def stored(values):
    return lax.optimization_barrier(values.astype(jnp.bfloat16)).astype(jnp.float32)

def recurrence_step(state, inputs):
    receptance, decay, key_row, value_row, unit_key, erase_dir = inputs
    removed = jnp.einsum('hij,hj->hi', state, -unit_key)
    state = state * decay[:, None, :] + removed[:, :, None] * erase_dir[:, None, :] + value_row[:, :, None] * key_row[:, None, :]
    return (state, jnp.einsum('hij,hj->hi', state, receptance))

def reference(tokens, input_norm_gain, convolution_value_weight, convolution_gate_weight, depthwise_taps_weight, convolution_group_gain, convolution_group_shift, receptance_weight, key_weight, value_weight, decay_weight, correction_rate_weight, output_gate_weight, key_prenorm_gain, decay_offset_bias, position_decay_shift, extra_log_decay, head_norm_gain, convolution_output_weight, attention_output_weight):
    float_rows = tokens.astype(jnp.float32)
    normed = (float_rows * lax.rsqrt(lax.optimization_barrier(jnp.mean(float_rows * float_rows, axis=-1, keepdims=True)) + NORM_EPS) * input_norm_gain).astype(jnp.bfloat16)

    def project(weight):
        return stored(jnp.dot(normed, weight, preferred_element_type=jnp.float32))
    conv_input = stored(project(convolution_value_weight) * jax.nn.sigmoid(project(convolution_gate_weight)))
    padded = jnp.pad(conv_input, ((CONV_TAPS - 1, 0), (0, 0)))
    conv_sum = jnp.zeros((TOKENS, CONV_CH), jnp.float32)
    for offset in range(CONV_TAPS):
        conv_sum = conv_sum + depthwise_taps_weight[offset] * padded[offset:offset + TOKENS]
    grouped = conv_sum.reshape(TOKENS, CONV_CH // 64, 64)
    centred = grouped - lax.optimization_barrier(jnp.mean(grouped, axis=-1, keepdims=True))
    grouped = centred * lax.rsqrt(lax.optimization_barrier(jnp.mean(centred * centred, axis=-1, keepdims=True)) + GROUP_EPS)
    conv_out = jax.nn.silu(grouped.reshape(TOKENS, CONV_CH) * convolution_group_gain + convolution_group_shift).astype(jnp.bfloat16)
    receptance = project(receptance_weight)
    key_all = project(key_weight)
    value_all = project(value_weight)
    decay_logits = project(decay_weight) + decay_offset_bias + position_decay_shift
    decay_logarithm = -jnp.exp(-jax.nn.softplus(-decay_logits) - 0.5) + extra_log_decay
    erase_rate = jax.nn.sigmoid(project(correction_rate_weight))
    out_gate = jax.nn.sigmoid(project(output_gate_weight))

    def by_head(values):
        return values.reshape(TOKENS, HEADS, HEAD)
    unit_key = by_head(key_all * key_prenorm_gain)
    unit_key = unit_key * lax.rsqrt(lax.optimization_barrier(jnp.sum(unit_key * unit_key, axis=-1, keepdims=True)) + KEY_EPS)
    erase_dir = unit_key * by_head(erase_rate)
    start_state = jnp.zeros((HEADS, HEAD, HEAD), jnp.float32)
    _, readout = lax.scan(recurrence_step, start_state, (by_head(receptance), by_head(jnp.exp(decay_logarithm)), by_head(key_all), by_head(value_all), unit_key, erase_dir))
    centred_read = readout - lax.optimization_barrier(jnp.mean(readout, axis=-1, keepdims=True))
    normed_read = centred_read * lax.rsqrt(lax.optimization_barrier(jnp.mean(centred_read * centred_read, axis=-1, keepdims=True)) + HEAD_EPS)
    mix_out = (normed_read.reshape(TOKENS, HEADS * HEAD) * head_norm_gain * out_gate).astype(jnp.bfloat16)
    projected = jnp.dot(conv_out, convolution_output_weight, preferred_element_type=jnp.float32) + jnp.dot(mix_out, attention_output_weight, preferred_element_type=jnp.float32)
    return projected.astype(jnp.bfloat16)
```

```python
import functools

import jax
import jax.numpy as jnp
from jax import lax
from jax.experimental import pallas as pl
from jax.experimental.pallas import tpu as pltpu
from jax.sharding import PartitionSpec as P

HEAD = 64
CHUNK = 64
PAIR = 128

NORM_EPS = 1e-06
GROUP_EPS = 1e-05
HEAD_EPS = 0.00064
KEY_EPS = 1e-06
MESH = pl.DeviceIdType.MESH
WIRE = jnp.bfloat16
VMEM_LIMIT = 60 * 1024 * 1024
F32 = jnp.float32
BF16 = jnp.bfloat16

NN = (((1,), (0,)), ((), ()))
NT = (((1,), (1,)), ((), ()))
TN = (((0,), (0,)), ((), ()))


def parts(x, count):
    out = []
    for _ in range(count - 1):
        piece = x.astype(BF16)
        out.append(piece)
        x = x - piece.astype(F32)
    out.append(x.astype(BF16))
    return out


def dot(a, b, dims=NN):
    return lax.dot_general(a, b, dims, preferred_element_type=F32)


def mm3(a, b, dims=NN):
    ah, al = parts(a, 2)
    bh, bl = parts(b, 2)
    return dot(ah, bh, dims) + (dot(ah, bl, dims) + dot(al, bh, dims))


def mm_left(a, b, dims=NN, count=2):
    pieces = [dot(piece, b, dims) for piece in parts(a, count)]
    return functools.reduce(jnp.add, pieces)


def mm_right(a, b, dims=NN, count=2):
    pieces = [dot(a, piece, dims) for piece in parts(b, count)]
    return functools.reduce(jnp.add, pieces)


def iota2(rows, cols):
    return (
        lax.broadcasted_iota(jnp.int32, (rows, cols), 0),
        lax.broadcasted_iota(jnp.int32, (rows, cols), 1),
    )


def head_blocks(width):
    row, col = iota2(width, width)
    return (row // HEAD) == (col // HEAD)


def block_diagonal(stacked, width):
    tiled = jnp.concatenate([stacked] * (width // HEAD), axis=0)
    return jnp.where(head_blocks(width), tiled, jnp.zeros_like(tiled))


def local_kernel(
    tok, gain, kgain, bias, shift, extra,
    wcv, wcg, wk, wr, wd, we, wv, wg,
    conv_in, local_out, carried_out, gate_out, tot,
    *scratch,
):
    sources = (wcv, wcg, wk, we, wd, wr, wv, wg)
    buffers, sem = scratch[:8], scratch[8]
    copies = []
    for index, (source, buffer) in enumerate(zip(sources, buffers)):
        copy = pltpu.make_async_copy(source, buffer, sem.at[index])
        copy.start()
        copies.append(copy)
    rows = tok.shape[0]
    width = local_out.shape[1]
    heads = width // HEAD
    pairs = rows // PAIR
    x = tok[...].astype(F32)
    normed = (
        x * lax.rsqrt(jnp.mean(x * x, axis=-1, keepdims=True) + NORM_EPS) * gain[...]
    ).astype(BF16)

    def project(index):
        copies[index].wait()
        return dot(normed, buffers[index][...]).astype(BF16).astype(F32)

    conv_value = project(0)
    conv_in[...] = (conv_value * jax.nn.sigmoid(project(1))).astype(BF16)
    key_all = project(2)
    ones = jnp.where(head_blocks(width), 1.0, 0.0).astype(BF16)
    unit = key_all * kgain[...]
    unit = unit * lax.rsqrt(mm_left(unit * unit, ones) + KEY_EPS)
    erase = unit * jax.nn.sigmoid(project(3))
    logits = project(4) + bias[...] + shift[...]
    decay = jax.nn.sigmoid(logits) * (-0.6065306597126334) + extra[...]
    row, col = iota2(PAIR, PAIR)
    same = (row // CHUNK) == (col // CHUNK)
    strict = same & (row > col)
    inclusive = same & (row >= col)
    eye = jnp.where(row == col, 1.0, 0.0)
    tri = jnp.where(inclusive, 1.0, 0.0).astype(BF16)
    cum = jnp.concatenate(
        [mm_right(tri, decay[p * PAIR:(p + 1) * PAIR], count=3) for p in range(pairs)], axis=0
    )

    def chunk_row(offset):
        return jnp.concatenate(
            [
                jnp.broadcast_to(cum[c + offset:c + offset + 1], (CHUNK, width))
                for c in range(0, rows, CHUNK)
            ],
            axis=0,
        )

    mid = chunk_row(CHUNK // 2 - 1)
    final = chunk_row(CHUNK - 1)
    before = cum - decay
    receptance = project(5)
    value = project(6)
    up = jnp.exp(mid - cum)
    left_unit = unit * jnp.exp(before - mid)
    left_read = receptance * jnp.exp(cum - mid)
    right_erase = erase * up
    right_key = key_all * up
    query_unit = unit * jnp.exp(before)
    query_read = receptance * jnp.exp(cum)
    keep = jnp.exp(final - cum)
    kept_erase = erase * keep
    kept_key = key_all * keep
    gate_out[...] = jax.nn.sigmoid(project(7))

    units = [(h, p) for h in range(heads) for p in range(pairs)]

    def piece(values, unit_index):
        h, p = unit_index
        return values[p * PAIR:(p + 1) * PAIR, h * HEAD:(h + 1) * HEAD]

    lower, read_mix, key_mix, values_of = [], [], [], []
    for u in units:
        left = jnp.concatenate([piece(left_unit, u), piece(left_read, u)], axis=0)
        right = jnp.concatenate([piece(right_erase, u), piece(right_key, u)], axis=0)
        product = mm3(left, right, NT)
        lower.append(jnp.where(strict, product[:PAIR, :PAIR], 0.0))
        key_mix.append(jnp.where(strict, product[:PAIR, PAIR:], 0.0))
        read_mix.append(
            jnp.concatenate(
                [
                    jnp.where(inclusive, product[PAIR:, :PAIR], 0.0),
                    jnp.where(inclusive, product[PAIR:, PAIR:], 0.0),
                ],
                axis=1,
            )
        )
        values_of.append(piece(value, u))
    right_side = [
        -jnp.concatenate([mm_left(k, v.astype(BF16)), piece(query_unit, u)], axis=1)
        for k, v, u in zip(key_mix, values_of, units)
    ]
    first = strict & ((row // 2) == (col // 2))
    inverse = [eye - jnp.where(first, low, 0.0) for low in lower]
    size = 2
    while size < CHUNK:
        level = ((row // (2 * size)) == (col // (2 * size))) & ((row // size) > (col // size))
        inner = [mm3(jnp.where(level, low, 0.0), inv) for low, inv in zip(lower, inverse)]
        inverse = [inv - mm3(inv, step) for inv, step in zip(inverse, inner)]
        size *= 2
    removed = [mm3(inv, rhs) for inv, rhs in zip(inverse, right_side)]
    zeros = jnp.zeros((PAIR, HEAD), F32)
    readout = []
    for mix, rem, val, u in zip(read_mix, removed, values_of, units):
        stacked = jnp.concatenate([rem, jnp.concatenate([val, zeros], axis=1)], axis=0)
        readout.append(
            mm3(mix, stacked) + jnp.concatenate([zeros, piece(query_read, u)], axis=1)
        )
    eye_head = iota2(HEAD, HEAD)
    eye_head = eye_head[0] == eye_head[1]
    for h in range(heads):
        state = None
        for p in range(pairs):
            index = h * pairs + p
            ke, kk = piece(kept_erase, (h, p)), piece(kept_key, (h, p))
            for half in range(PAIR // CHUNK):
                span = slice(half * CHUNK, (half + 1) * CHUNK)
                start = p * PAIR + half * CHUNK
                lanes = slice(h * HEAD, (h + 1) * HEAD)
                read = readout[index][span]
                if state is not None:
                    read = jnp.concatenate(
                        [read[:, :HEAD], jnp.zeros((CHUNK, HEAD), F32)], axis=1
                    ) + mm3(read[:, HEAD:], state, NT)
                local_out[start:start + CHUNK, lanes] = read[:, :HEAD]
                carried_out[start:start + CHUNK, lanes] = read[:, HEAD:]
                from_removed = mm3(removed[index][span], ke[span], TN)
                base = from_removed[:HEAD] + mm3(values_of[index][span], kk[span], TN)
                last = jnp.exp(final[start:start + 1, lanes])
                trans = from_removed[HEAD:] + jnp.where(eye_head, last, 0.0)
                if state is None:
                    state = jnp.concatenate([base, trans], axis=0)
                else:
                    moved = mm3(state, trans)
                    state = jnp.concatenate([moved[:HEAD] + base, moved[HEAD:]], axis=0)
        tot[:, h * HEAD:(h + 1) * HEAD] = state.astype(tot.dtype)


def exchange_kernel(
    n_sp, n_tp,
    conv_in, taps, ggain, gshift, local_read, carried, gate, tot, hgain, wco, wao,
    out,
    wco_buf, wao_buf, extended, halo, partner_map, pair_map, maps, state,
    conv_out, mix_out, conv_slots, mix_slots,
    weight_sem, halo_sem, pair_sem, map_send, map_recv, conv_send, conv_recv, mix_send, mix_recv,
):
    sp, tp = lax.axis_index("sp"), lax.axis_index("tp")
    weight_copies = [
        pltpu.make_async_copy(wco, wco_buf, weight_sem.at[0]),
        pltpu.make_async_copy(wao, wao_buf, weight_sem.at[1]),
    ]
    for copy in weight_copies:
        copy.start()
    barrier = pltpu.get_barrier_semaphore()
    for step in range(1, n_sp):
        pl.semaphore_signal(
            barrier, inc=1, device_id=(lax.rem(sp + step, n_sp), tp), device_id_type=MESH
        )
    for step in range(1, n_tp):
        pl.semaphore_signal(
            barrier, inc=1, device_id=(sp, lax.rem(tp + step, n_tp)), device_id_type=MESH
        )
    pl.semaphore_wait(barrier, n_sp + n_tp - 2)

    rows, channels = conv_in.shape
    width = local_read.shape[1]
    halo_rows = halo.shape[0]
    groups = n_sp // 2
    group, parity = sp // 2, lax.rem(sp, 2)
    first_member = parity == 0

    pair_copy = pltpu.make_async_remote_copy(
        src_ref=tot, dst_ref=partner_map, send_sem=pair_sem.at[0], recv_sem=pair_sem.at[1],
        device_id=(sp + 1 - 2 * parity, tp), device_id_type=MESH,
    )
    pair_copy.start()
    halo_copy = pltpu.make_async_remote_copy(
        src_ref=conv_in.at[pl.ds(rows - halo_rows, halo_rows)], dst_ref=halo,
        send_sem=halo_sem.at[0], recv_sem=halo_sem.at[1],
        device_id=(lax.rem(sp + 1, n_sp), tp), device_id_type=MESH,
    )
    halo_copy.start()
    extended[halo_rows:, :] = conv_in[...].astype(F32)

    def chain(carry, block):
        trans = block_diagonal(block[HEAD:].astype(F32), width).astype(BF16)
        return mm_left(carry, trans) if WIRE == BF16 else mm3(
            carry, block_diagonal(block[HEAD:].astype(F32), width))

    pair_copy.wait()
    mine, theirs = tot[...].astype(F32), partner_map[...].astype(F32)
    early = jnp.where(first_member, mine, theirs)
    late = jnp.where(first_member, theirs, mine)
    joined = chain(early, late)
    pair_map[:HEAD] = (joined[:HEAD] + late[:HEAD]).astype(pair_map.dtype)
    pair_map[HEAD:] = joined[HEAD:].astype(pair_map.dtype)

    def map_copy(ahead):
        return pltpu.make_async_remote_copy(
            src_ref=pair_map, dst_ref=maps.at[ahead],
            send_sem=map_send.at[ahead], recv_sem=map_recv.at[ahead],
            device_id=(sp + 2 * ahead, tp), device_id_type=MESH,
        )

    for ahead in range(1, groups):
        @pl.when(group + ahead < groups)
        def _():
            map_copy(ahead).start()

    halo_copy.wait()
    received = halo[...].astype(F32)
    extended[:halo_rows, :] = jnp.where(sp == 0, 0.0, received)
    tap_count = taps.shape[0]
    total = jnp.zeros((rows, channels), F32)
    for offset in range(tap_count):
        begin = halo_rows - tap_count + 1 + offset
        total = total + taps[offset:offset + 1, :] * extended[begin:begin + rows, :]
    means = jnp.where(head_blocks(channels), 1.0 / HEAD, 0.0).astype(BF16)
    centred = total - mm_left(total, means)
    scaled = centred * lax.rsqrt(mm_left(centred * centred, means) + GROUP_EPS)
    conv_out[...] = jax.nn.silu(scaled * ggain[...] + gshift[...]).astype(BF16)

    span = rows // n_tp

    def spread(source, slots, send, recv):
        copies = []
        for step in range(1, n_tp):
            target = lax.rem(tp + step, n_tp)
            begin = pl.multiple_of(target * span, span)
            copy = pltpu.make_async_remote_copy(
                src_ref=source.at[pl.ds(begin, span)], dst_ref=slots.at[step],
                send_sem=send.at[step], recv_sem=recv.at[step],
                device_id=(sp, target), device_id_type=MESH,
            )
            copy.start()
            copies.append(copy)
        return copies

    conv_copies = spread(conv_out, conv_slots, conv_send, conv_recv)

    state[...] = jnp.zeros_like(state)
    for ahead in range(groups - 1, 0, -1):
        @pl.when(group >= ahead)
        def _():
            map_copy(ahead).wait_recv()
            block = maps[ahead]
            state[...] = chain(state[...], block) + block[:HEAD].astype(F32)

    behind = chain(state[...], early) + early[:HEAD]
    entering = jnp.where(first_member, state[...], behind)
    readout = local_read[...] + mm3(carried[...], block_diagonal(entering, width), NT)
    head_means = jnp.where(head_blocks(width), 1.0 / HEAD, 0.0).astype(BF16)
    centred = readout - mm_left(readout, head_means)
    scaled = centred * lax.rsqrt(mm_left(centred * centred, head_means) + HEAD_EPS)
    mix_out[...] = (scaled * hgain[...] * gate[...]).astype(BF16)
    mix_copies = spread(mix_out, mix_slots, mix_send, mix_recv)

    own = pl.multiple_of(tp * span, span)
    for copy in weight_copies:
        copy.wait()

    def gather(result, source, slots, copies, weight, depth):
        result = result + dot(
            source[pl.ds(own, span)], weight[pl.ds(pl.multiple_of(tp * depth, depth), depth)]
        )
        for step in range(1, n_tp):
            copies[step - 1].wait_recv()
            begin = lax.rem(tp - step + n_tp, n_tp) * depth
            result = result + dot(
                slots[step], weight[pl.ds(pl.multiple_of(begin, depth), depth)]
            )
        return result

    result = gather(
        jnp.zeros(out.shape, F32), conv_out, conv_slots, conv_copies, wco_buf, channels
    )
    result = gather(result, mix_out, mix_slots, mix_copies, wao_buf, width)
    out[...] = result.astype(BF16)
    for copy in conv_copies + mix_copies:
        copy.wait_send()
    for ahead in range(1, groups):
        @pl.when(group + ahead < groups)
        def _():
            map_copy(ahead).wait_send()


def local(
    n_sp, n_tp,
    tokens, input_norm_gain, convolution_value_weight, convolution_gate_weight,
    depthwise_taps_weight, convolution_group_gain, convolution_group_shift,
    receptance_weight, key_weight, value_weight, decay_weight, correction_rate_weight,
    output_gate_weight, key_prenorm_gain, decay_offset_bias, position_decay_shift,
    extra_log_decay, head_norm_gain, convolution_output_weight, attention_output_weight,
):
    rows, model = tokens.shape
    channels = convolution_value_weight.shape[1]
    width = key_weight.shape[1]
    vmem = pl.BlockSpec(memory_space=pltpu.VMEM)
    anywhere = pl.BlockSpec(memory_space=pl.ANY)

    def line(values):
        return values.reshape(1, -1)

    weight_shapes = [(model, channels)] * 2 + [(model, width)] * 6
    conv_in, local_read, carried, gate, tot = pl.pallas_call(
        local_kernel,
        name="local_pass",
        out_shape=(
            jax.ShapeDtypeStruct((rows, channels), BF16),
            jax.ShapeDtypeStruct((rows, width), F32),
            jax.ShapeDtypeStruct((rows, width), F32),
            jax.ShapeDtypeStruct((rows, width), F32),
            jax.ShapeDtypeStruct((2 * HEAD, width), WIRE),
        ),
        in_specs=[vmem] * 6 + [anywhere] * 8,
        out_specs=(vmem,) * 5,
        scratch_shapes=[pltpu.VMEM(shape, BF16) for shape in weight_shapes]
        + [pltpu.SemaphoreType.DMA((8,))],
        compiler_params=pltpu.CompilerParams(vmem_limit_bytes=VMEM_LIMIT),
    )(
        tokens, line(input_norm_gain), line(key_prenorm_gain), line(decay_offset_bias),
        position_decay_shift, extra_log_decay,
        convolution_value_weight, convolution_gate_weight, key_weight, receptance_weight,
        decay_weight, correction_rate_weight, value_weight, output_gate_weight,
    )
    span = rows // n_tp
    halo_rows = -(-(depthwise_taps_weight.shape[0] - 1) // 16) * 16
    groups = n_sp // 2
    dma = pltpu.SemaphoreType.DMA
    return pl.pallas_call(
        functools.partial(exchange_kernel, n_sp, n_tp),
        name="exchange_pass",
        out_shape=jax.ShapeDtypeStruct((span, model), BF16),
        in_specs=[vmem] * 9 + [anywhere] * 2,
        out_specs=vmem,
        scratch_shapes=[
            pltpu.VMEM(convolution_output_weight.shape, BF16),
            pltpu.VMEM(attention_output_weight.shape, BF16),
            pltpu.VMEM((halo_rows + rows, channels), F32),
            pltpu.VMEM((halo_rows, channels), BF16),
            pltpu.VMEM((2 * HEAD, width), WIRE),
            pltpu.VMEM((2 * HEAD, width), WIRE),
            pltpu.VMEM((groups, 2 * HEAD, width), WIRE),
            pltpu.VMEM((HEAD, width), F32),
            pltpu.VMEM((rows, channels), BF16),
            pltpu.VMEM((rows, width), BF16),
            pltpu.VMEM((n_tp, span, channels), BF16),
            pltpu.VMEM((n_tp, span, width), BF16),
            dma((2,)), dma((2,)), dma((2,)), dma((groups,)), dma((groups,)),
            dma((n_tp,)), dma((n_tp,)), dma((n_tp,)), dma((n_tp,)),
        ],
        compiler_params=pltpu.CompilerParams(
            collective_id=0, has_side_effects=True, vmem_limit_bytes=VMEM_LIMIT
        ),
    )(
        conv_in, depthwise_taps_weight, line(convolution_group_gain),
        line(convolution_group_shift), local_read, carried, gate, tot, line(head_norm_gain),
        convolution_output_weight, attention_output_weight,
    )


def solution(mesh):
    in_specs = (
        P("sp", None),
        P(),
        P(None, "tp"),
        P(None, "tp"),
        P(None, "tp"),
        P("tp"),
        P("tp"),
        P(None, "tp"),
        P(None, "tp"),
        P(None, "tp"),
        P(None, "tp"),
        P(None, "tp"),
        P(None, "tp"),
        P("tp"),
        P("tp"),
        P("sp", "tp"),
        P("sp", "tp"),
        P("tp"),
        P(),
        P(),
    )
    body = functools.partial(local, mesh.shape["sp"], mesh.shape["tp"])
    return jax.shard_map(
        body, mesh=mesh, in_specs=in_specs, out_specs=P(("sp", "tp"), None), check_vma=False
    )
```

```python
import functools

import jax
import jax.numpy as jnp
from jax import lax
from jax.experimental import pallas as pl
from jax.experimental.pallas import tpu as pltpu
from jax.sharding import PartitionSpec as P

HEAD = 64
CHUNK = 64
PAIR = 128

NORM_EPS = 1e-06
GROUP_EPS = 1e-05
HEAD_EPS = 0.00064
KEY_EPS = 1e-06
MESH = pl.DeviceIdType.MESH
WIRE = jnp.bfloat16
VMEM_LIMIT = 60 * 1024 * 1024
F32 = jnp.float32
BF16 = jnp.bfloat16

NN = (((1,), (0,)), ((), ()))
NT = (((1,), (1,)), ((), ()))
TN = (((0,), (0,)), ((), ()))


def parts(x, count):
    out = []
    for _ in range(count - 1):
        piece = x.astype(BF16)
        out.append(piece)
        x = x - piece.astype(F32)
    out.append(x.astype(BF16))
    return out


def dot(a, b, dims=NN):
    return lax.dot_general(a, b, dims, preferred_element_type=F32)


def mm3(a, b, dims=NN):
    ah, al = parts(a, 2)
    bh, bl = parts(b, 2)
    return dot(ah, bh, dims) + (dot(ah, bl, dims) + dot(al, bh, dims))


def mm_left(a, b, dims=NN, count=2):
    pieces = [dot(piece, b, dims) for piece in parts(a, count)]
    return functools.reduce(jnp.add, pieces)


def mm_right(a, b, dims=NN, count=2):
    pieces = [dot(a, piece, dims) for piece in parts(b, count)]
    return functools.reduce(jnp.add, pieces)


PASSES = dict(qk=3, kmv=2, inv=1, rem=1, res=3, fix=1, read=3, keep=3, state=3, carry=3, enter=3)
REFINE = True


def mm(a, b, site, dims=NN):
    passes = PASSES[site]
    if passes == 1:
        return dot(a.astype(BF16), b.astype(BF16), dims)
    if passes == 2:
        return mm_left(a, b.astype(BF16), dims)
    return mm3(a, b, dims)


def iota2(rows, cols):
    return (
        lax.broadcasted_iota(jnp.int32, (rows, cols), 0),
        lax.broadcasted_iota(jnp.int32, (rows, cols), 1),
    )


def head_blocks(width):
    row, col = iota2(width, width)
    return (row // HEAD) == (col // HEAD)


def block_diagonal(stacked, width):
    tiled = jnp.concatenate([stacked] * (width // HEAD), axis=0)
    return jnp.where(head_blocks(width), tiled, jnp.zeros_like(tiled))


def layer_kernel(
    n_sp, n_tp,
    tok, gain, kgain, bias, shift, extra, taps, ggain, gshift, hgain,
    wcv, wcg, wk, wr, wd, we, wv, wg, wco, wao,
    out,
    cv_buf, cg_buf, k_buf, r_buf, d_buf, e_buf, v_buf, g_buf, co_buf, ao_buf,
    conv_in, extended, halo, own_map, partner_map, pair_map, maps, state,
    local_read, carried, conv_out, mix_out, conv_slots, mix_slots,
    weight_sem, halo_sem, pair_sem, map_send, map_recv, conv_send, conv_recv, mix_send, mix_recv,
):
    sp, tp = lax.axis_index("sp"), lax.axis_index("tp")
    barrier = pltpu.get_barrier_semaphore()
    for step in range(1, n_sp):
        pl.semaphore_signal(
            barrier, inc=1, device_id=(lax.rem(sp + step, n_sp), tp), device_id_type=MESH
        )
    for step in range(1, n_tp):
        pl.semaphore_signal(
            barrier, inc=1, device_id=(sp, lax.rem(tp + step, n_tp)), device_id_type=MESH
        )
    order = (
        (wk, k_buf), (we, e_buf), (wd, d_buf), (wv, v_buf), (wcv, cv_buf), (wcg, cg_buf),
        (wr, r_buf), (wg, g_buf), (wco, co_buf), (wao, ao_buf),
    )
    copies = []
    for index, (source, buffer) in enumerate(order):
        copy = pltpu.make_async_copy(source, buffer, weight_sem.at[index])
        copy.start()
        copies.append(copy)
    rows = tok.shape[0]
    channels = conv_in.shape[1]
    width = local_read.shape[1]
    heads = width // HEAD
    pairs = rows // PAIR
    halo_rows = halo.shape[0]
    groups = n_sp // 2
    group, parity = sp // 2, lax.rem(sp, 2)
    first_member = parity == 0
    x = tok[...].astype(F32)
    normed = (
        x * lax.rsqrt(jnp.mean(x * x, axis=-1, keepdims=True) + NORM_EPS) * gain[...]
    ).astype(BF16)

    def project(index):
        copies[index].wait()
        return dot(normed, order[index][1][...]).astype(BF16).astype(F32)

    key_all = project(0)
    ones = jnp.where(head_blocks(width), 1.0, 0.0).astype(BF16)
    unit = key_all * kgain[...]
    unit = unit * lax.rsqrt(mm_left(unit * unit, ones) + KEY_EPS)
    erase = unit * jax.nn.sigmoid(project(1))
    logits = project(2) + bias[...] + shift[...]
    decay = jax.nn.sigmoid(logits) * (-0.6065306597126334) + extra[...]
    row, col = iota2(PAIR, PAIR)
    same = (row // CHUNK) == (col // CHUNK)
    strict = same & (row > col)
    inclusive = same & (row >= col)
    eye = jnp.where(row == col, 1.0, 0.0)
    tri = jnp.where(inclusive, 1.0, 0.0).astype(BF16)
    cum = jnp.concatenate(
        [mm_right(tri, decay[p * PAIR:(p + 1) * PAIR], count=3) for p in range(pairs)], axis=0
    )

    def chunk_row(offset):
        return jnp.concatenate(
            [
                jnp.broadcast_to(cum[c + offset:c + offset + 1], (CHUNK, width))
                for c in range(0, rows, CHUNK)
            ],
            axis=0,
        )

    mid = chunk_row(CHUNK // 2 - 1)
    final = chunk_row(CHUNK - 1)
    before = cum - decay
    up = jnp.exp(mid - cum)
    left_unit = unit * jnp.exp(before - mid)
    right_erase = erase * up
    right_key = key_all * up
    query_unit = unit * jnp.exp(before)
    keep = jnp.exp(final - cum)
    kept_erase = erase * keep
    kept_key = key_all * keep
    value = project(3)

    units = [(h, p) for h in range(heads) for p in range(pairs)]

    def piece(values, unit_index):
        h, p = unit_index
        return values[p * PAIR:(p + 1) * PAIR, h * HEAD:(h + 1) * HEAD]

    lower, key_mix, values_of, rights = [], [], [], []
    for u in units:
        right = jnp.concatenate([piece(right_erase, u), piece(right_key, u)], axis=0)
        product = mm(piece(left_unit, u), right, "qk", NT)
        lower.append(jnp.where(strict, product[:, :PAIR], 0.0))
        key_mix.append(jnp.where(strict, product[:, PAIR:], 0.0))
        values_of.append(piece(value, u))
        rights.append(right)
    right_side = [
        -jnp.concatenate([mm(k, v, "kmv"), piece(query_unit, u)], axis=1)
        for k, v, u in zip(key_mix, values_of, units)
    ]
    first = strict & ((row // 2) == (col // 2))
    inverse = [eye - jnp.where(first, low, 0.0) for low in lower]
    size = 2
    while size < CHUNK:
        level = ((row // (2 * size)) == (col // (2 * size))) & ((row // size) > (col // size))
        inner = [mm(jnp.where(level, low, 0.0), inv, "inv") for low, inv in zip(lower, inverse)]
        inverse = [inv - mm(inv, step, "inv") for inv, step in zip(inverse, inner)]
        size *= 2
    removed = [mm(inv, rhs, "rem") for inv, rhs in zip(inverse, right_side)]
    if REFINE:
        left_over = [
            rhs - rem - mm(low, rem, "res") for rhs, rem, low in zip(right_side, removed, lower)
        ]
        removed = [
            rem + mm(inv, rest, "fix") for rem, inv, rest in zip(removed, inverse, left_over)
        ]
    eye_head = iota2(HEAD, HEAD)
    eye_head = eye_head[0] == eye_head[1]
    blocks = {}
    for h in range(heads):
        for p in range(pairs):
            index = h * pairs + p
            ke, kk = piece(kept_erase, (h, p)), piece(kept_key, (h, p))
            for half in range(PAIR // CHUNK):
                span = slice(half * CHUNK, (half + 1) * CHUNK)
                start = p * PAIR + half * CHUNK
                from_removed = mm(removed[index][span], ke[span], "keep", TN)
                base = from_removed[:HEAD] + mm(values_of[index][span], kk[span], "keep", TN)
                last = jnp.exp(final[start:start + 1, h * HEAD:(h + 1) * HEAD])
                trans = from_removed[HEAD:] + jnp.where(eye_head, last, 0.0)
                blocks[h, start // CHUNK] = (base, trans)
    priors = {}
    totals = [None] * heads
    for chunk in range(rows // CHUNK):
        for h in range(heads):
            base, trans = blocks[h, chunk]
            priors[h, chunk] = totals[h]
            if totals[h] is None:
                totals[h] = jnp.concatenate([base, trans], axis=0)
            else:
                moved = mm(totals[h], trans, "state")
                totals[h] = jnp.concatenate([moved[:HEAD] + base, moved[HEAD:]], axis=0)
    own_total = jnp.concatenate(totals, axis=1).astype(WIRE)
    own_map[...] = own_total

    pl.semaphore_wait(barrier, n_sp + n_tp - 2)
    pair_copy = pltpu.make_async_remote_copy(
        src_ref=own_map, dst_ref=partner_map, send_sem=pair_sem.at[0], recv_sem=pair_sem.at[1],
        device_id=(sp + 1 - 2 * parity, tp), device_id_type=MESH,
    )
    pair_copy.start()

    conv_value = project(4)
    conv_rows = (conv_value * jax.nn.sigmoid(project(5))).astype(BF16)
    conv_in[...] = conv_rows
    halo_copy = pltpu.make_async_remote_copy(
        src_ref=conv_in.at[pl.ds(rows - halo_rows, halo_rows)], dst_ref=halo,
        send_sem=halo_sem.at[0], recv_sem=halo_sem.at[1],
        device_id=(lax.rem(sp + 1, n_sp), tp), device_id_type=MESH,
    )
    halo_copy.start()
    extended[halo_rows:, :] = conv_rows.astype(F32)

    def chain(carry, block):
        trans = block_diagonal(block[HEAD:], width)
        return mm(carry, trans, "enter")

    receptance = project(6)
    left_read = receptance * jnp.exp(cum - mid)
    query_read = receptance * jnp.exp(cum)

    pair_copy.wait()
    mine, theirs = own_total.astype(F32), partner_map[...].astype(F32)
    early = jnp.where(first_member, mine, theirs)
    late = jnp.where(first_member, theirs, mine)
    joined = chain(early, late)
    pair_map[:HEAD] = (joined[:HEAD] + late[:HEAD]).astype(WIRE)
    pair_map[HEAD:] = joined[HEAD:].astype(WIRE)

    def map_copy(ahead):
        return pltpu.make_async_remote_copy(
            src_ref=pair_map, dst_ref=maps.at[ahead],
            send_sem=map_send.at[ahead], recv_sem=map_recv.at[ahead],
            device_id=(sp + 2 * ahead, tp), device_id_type=MESH,
        )

    for ahead in range(1, groups):
        @pl.when(group + ahead < groups)
        def _():
            map_copy(ahead).start()

    halo_copy.wait()
    received = halo[...].astype(F32)
    extended[:halo_rows, :] = jnp.where(sp == 0, 0.0, received)
    tap_count = taps.shape[0]
    total = jnp.zeros((rows, channels), F32)
    for offset in range(tap_count):
        begin = halo_rows - tap_count + 1 + offset
        total = total + taps[offset:offset + 1, :] * extended[begin:begin + rows, :]
    means = jnp.where(head_blocks(channels), 1.0 / HEAD, 0.0).astype(BF16)
    centred = total - mm_left(total, means)
    scaled = centred * lax.rsqrt(mm_left(centred * centred, means) + GROUP_EPS)
    conv_out[...] = jax.nn.silu(scaled * ggain[...] + gshift[...]).astype(BF16)

    span = rows // n_tp

    def spread(source, slots, send, recv):
        started = []
        for step in range(1, n_tp):
            target = lax.rem(tp + step, n_tp)
            begin = pl.multiple_of(target * span, span)
            copy = pltpu.make_async_remote_copy(
                src_ref=source.at[pl.ds(begin, span)], dst_ref=slots.at[step],
                send_sem=send.at[step], recv_sem=recv.at[step],
                device_id=(sp, target), device_id_type=MESH,
            )
            copy.start()
            started.append(copy)
        return started

    conv_copies = spread(conv_out, conv_slots, conv_send, conv_recv)

    zeros = jnp.zeros((PAIR, HEAD), F32)
    for index, u in enumerate(units):
        h, p = u
        product = mm(piece(left_read, u), rights[index], "qk", NT)
        mix = jnp.concatenate(
            [
                jnp.where(inclusive, product[:, :PAIR], 0.0),
                jnp.where(inclusive, product[:, PAIR:], 0.0),
            ],
            axis=1,
        )
        stacked = jnp.concatenate(
            [removed[index], jnp.concatenate([values_of[index], zeros], axis=1)], axis=0
        )
        readout = mm(mix, stacked, "read") + jnp.concatenate(
            [zeros, piece(query_read, u)], axis=1
        )
        for half in range(PAIR // CHUNK):
            start = p * PAIR + half * CHUNK
            lanes = slice(h * HEAD, (h + 1) * HEAD)
            read = readout[half * CHUNK:(half + 1) * CHUNK]
            prior = priors[h, start // CHUNK]
            if prior is not None:
                read = jnp.concatenate(
                    [read[:, :HEAD], jnp.zeros((CHUNK, HEAD), F32)], axis=1
                ) + mm(read[:, HEAD:], prior, "carry", NT)
            local_read[start:start + CHUNK, lanes] = read[:, :HEAD]
            carried[start:start + CHUNK, lanes] = read[:, HEAD:]
    gate = jax.nn.sigmoid(project(7)) * hgain[...]

    own = pl.multiple_of(tp * span, span)

    def gather(result, source, slots, arriving, weight, depth):
        result = result + dot(
            source[pl.ds(own, span)], weight[pl.ds(pl.multiple_of(tp * depth, depth), depth)]
        )
        for step in range(1, n_tp):
            arriving[step - 1].wait_recv()
            begin = lax.rem(tp - step + n_tp, n_tp) * depth
            result = result + dot(
                slots[step], weight[pl.ds(pl.multiple_of(begin, depth), depth)]
            )
        return result

    copies[8].wait()
    result = gather(
        jnp.zeros(out.shape, F32), conv_out, conv_slots, conv_copies, co_buf, channels
    )

    state[...] = jnp.zeros_like(state)
    for ahead in range(groups - 1, 0, -1):
        @pl.when(group >= ahead)
        def _():
            map_copy(ahead).wait_recv()
            block = maps[ahead].astype(F32)
            state[...] = chain(state[...], block) + block[:HEAD]

    behind = chain(state[...], early) + early[:HEAD]
    entering = jnp.where(first_member, state[...], behind)
    readout = local_read[...] + mm(carried[...], block_diagonal(entering, width), "enter", NT)
    head_means = jnp.where(head_blocks(width), 1.0 / HEAD, 0.0).astype(BF16)
    centred = readout - mm_left(readout, head_means)
    scaled = centred * lax.rsqrt(mm_left(centred * centred, head_means) + HEAD_EPS)
    mix_out[...] = (scaled * gate).astype(BF16)
    mix_copies = spread(mix_out, mix_slots, mix_send, mix_recv)
    copies[9].wait()
    result = gather(result, mix_out, mix_slots, mix_copies, ao_buf, width)
    out[...] = result.astype(BF16)
    for copy in conv_copies + mix_copies:
        copy.wait_send()
    for ahead in range(1, groups):
        @pl.when(group + ahead < groups)
        def _():
            map_copy(ahead).wait_send()


def local(
    n_sp, n_tp,
    tokens, input_norm_gain, convolution_value_weight, convolution_gate_weight,
    depthwise_taps_weight, convolution_group_gain, convolution_group_shift,
    receptance_weight, key_weight, value_weight, decay_weight, correction_rate_weight,
    output_gate_weight, key_prenorm_gain, decay_offset_bias, position_decay_shift,
    extra_log_decay, head_norm_gain, convolution_output_weight, attention_output_weight,
):
    rows, model = tokens.shape
    channels = convolution_value_weight.shape[1]
    width = key_weight.shape[1]
    vmem = pl.BlockSpec(memory_space=pltpu.VMEM)
    anywhere = pl.BlockSpec(memory_space=pl.ANY)

    def line(values):
        return values.reshape(1, -1)

    weights = (
        convolution_value_weight, convolution_gate_weight, key_weight, receptance_weight,
        decay_weight, correction_rate_weight, value_weight, output_gate_weight,
        convolution_output_weight, attention_output_weight,
    )
    span = rows // n_tp
    halo_rows = -(-(depthwise_taps_weight.shape[0] - 1) // 16) * 16
    groups = n_sp // 2
    dma = pltpu.SemaphoreType.DMA
    map_shape = (2 * HEAD, width)
    return pl.pallas_call(
        functools.partial(layer_kernel, n_sp, n_tp),
        name="layer",
        out_shape=jax.ShapeDtypeStruct((span, model), BF16),
        in_specs=[vmem] * 10 + [anywhere] * 10,
        out_specs=vmem,
        scratch_shapes=[pltpu.VMEM(weight.shape, BF16) for weight in weights]
        + [
            pltpu.VMEM((rows, channels), BF16),
            pltpu.VMEM((halo_rows + rows, channels), F32),
            pltpu.VMEM((halo_rows, channels), BF16),
            pltpu.VMEM(map_shape, WIRE),
            pltpu.VMEM(map_shape, WIRE),
            pltpu.VMEM(map_shape, WIRE),
            pltpu.VMEM((groups,) + map_shape, WIRE),
            pltpu.VMEM((HEAD, width), F32),
            pltpu.VMEM((rows, width), F32),
            pltpu.VMEM((rows, width), F32),
            pltpu.VMEM((rows, channels), BF16),
            pltpu.VMEM((rows, width), BF16),
            pltpu.VMEM((n_tp, span, channels), BF16),
            pltpu.VMEM((n_tp, span, width), BF16),
            dma((10,)), dma((2,)), dma((2,)), dma((groups,)), dma((groups,)),
            dma((n_tp,)), dma((n_tp,)), dma((n_tp,)), dma((n_tp,)),
        ],
        compiler_params=pltpu.CompilerParams(
            collective_id=0, has_side_effects=True, vmem_limit_bytes=VMEM_LIMIT
        ),
    )(
        tokens, line(input_norm_gain), line(key_prenorm_gain), line(decay_offset_bias),
        position_decay_shift, extra_log_decay, depthwise_taps_weight,
        line(convolution_group_gain), line(convolution_group_shift), line(head_norm_gain),
        *weights,
    )


def solution(mesh):
    in_specs = (
        P("sp", None),
        P(),
        P(None, "tp"),
        P(None, "tp"),
        P(None, "tp"),
        P("tp"),
        P("tp"),
        P(None, "tp"),
        P(None, "tp"),
        P(None, "tp"),
        P(None, "tp"),
        P(None, "tp"),
        P(None, "tp"),
        P("tp"),
        P("tp"),
        P("sp", "tp"),
        P("sp", "tp"),
        P("tp"),
        P(),
        P(),
    )
    body = functools.partial(local, mesh.shape["sp"], mesh.shape["tp"])
    return jax.shard_map(
        body, mesh=mesh, in_specs=in_specs, out_specs=P(("sp", "tp"), None), check_vma=False
    )
```

```python
import functools

import jax
import jax.numpy as jnp
from jax import lax
from jax.experimental import pallas as pl
from jax.experimental.pallas import tpu as pltpu
from jax.sharding import PartitionSpec as P

HEAD = 64
CHUNK = 64
PAIR = 128

NORM_EPS = 1e-06
GROUP_EPS = 1e-05
HEAD_EPS = 0.00064
KEY_EPS = 1e-06
MESH = pl.DeviceIdType.MESH
WIRE = jnp.bfloat16
VMEM_LIMIT = 60 * 1024 * 1024
F32 = jnp.float32
BF16 = jnp.bfloat16

NN = (((1,), (0,)), ((), ()))
NT = (((1,), (1,)), ((), ()))
TN = (((0,), (0,)), ((), ()))


def parts(x, count):
    out = []
    for _ in range(count - 1):
        piece = x.astype(BF16)
        out.append(piece)
        x = x - piece.astype(F32)
    out.append(x.astype(BF16))
    return out


def dot(a, b, dims=NN):
    return lax.dot_general(a, b, dims, preferred_element_type=F32)


def mm3(a, b, dims=NN):
    ah, al = parts(a, 2)
    bh, bl = parts(b, 2)
    return dot(ah, bh, dims) + (dot(ah, bl, dims) + dot(al, bh, dims))


def mm_left(a, b, dims=NN, count=2):
    pieces = [dot(piece, b, dims) for piece in parts(a, count)]
    return functools.reduce(jnp.add, pieces)


def mm_right(a, b, dims=NN, count=2):
    pieces = [dot(a, piece, dims) for piece in parts(b, count)]
    return functools.reduce(jnp.add, pieces)


PASSES = dict(qk=3, kmv=2, inv=1, rem=1, res=3, fix=1, read=3, keep=3, state=3, carry=3, enter=3)
REFINE = True


def mm(a, b, site, dims=NN):
    passes = PASSES[site]
    if passes == 1:
        return dot(a.astype(BF16), b.astype(BF16), dims)
    if passes == 2:
        return mm_left(a, b.astype(BF16), dims)
    return mm3(a, b, dims)


def iota2(rows, cols):
    return (
        lax.broadcasted_iota(jnp.int32, (rows, cols), 0),
        lax.broadcasted_iota(jnp.int32, (rows, cols), 1),
    )


def head_blocks(width):
    row, col = iota2(width, width)
    return (row // HEAD) == (col // HEAD)


def block_diagonal(stacked, width):
    tiled = jnp.concatenate([stacked] * (width // HEAD), axis=0)
    return jnp.where(head_blocks(width), tiled, jnp.zeros_like(tiled))


def layer_kernel(
    n_sp, n_tp,
    gain, kgain, bias, taps, ggain, gshift, hgain,
    tok_hbm, shift_hbm, extra_hbm, wcv, wcg, wk, wr, wd, we, wv, wg, wco, wao,
    out,
    tok, shift, extra, cv_buf, cg_buf, k_buf, r_buf, d_buf, e_buf, v_buf, g_buf, co_buf, ao_buf,
    conv_in, extended, halo, own_map, partner_map, pair_map, maps, state,
    local_read, carried, conv_out, mix_out, conv_slots, mix_slots,
    weight_sem, halo_sem, pair_sem, map_send, map_recv, conv_send, conv_recv, mix_send, mix_recv,
):
    sp, tp = lax.axis_index("sp"), lax.axis_index("tp")
    order = (
        (tok_hbm, tok), (wk, k_buf), (we, e_buf), (shift_hbm, shift), (extra_hbm, extra),
        (wd, d_buf), (wv, v_buf), (wcv, cv_buf), (wcg, cg_buf),
        (wr, r_buf), (wg, g_buf), (wco, co_buf), (wao, ao_buf),
    )
    copies = []
    for index, (source, buffer) in enumerate(order):
        copy = pltpu.make_async_copy(source, buffer, weight_sem.at[index])
        copy.start()
        copies.append(copy)
    barrier = pltpu.get_barrier_semaphore()
    for step in range(1, n_sp):
        pl.semaphore_signal(
            barrier, inc=1, device_id=(lax.rem(sp + step, n_sp), tp), device_id_type=MESH
        )
    for step in range(1, n_tp):
        pl.semaphore_signal(
            barrier, inc=1, device_id=(sp, lax.rem(tp + step, n_tp)), device_id_type=MESH
        )
    rows = tok.shape[0]
    channels = conv_in.shape[1]
    width = local_read.shape[1]
    heads = width // HEAD
    pairs = rows // PAIR
    halo_rows = halo.shape[0]
    groups = n_sp // 2
    group, parity = sp // 2, lax.rem(sp, 2)
    first_member = parity == 0
    copies[0].wait()
    x = tok[...].astype(F32)
    normed = (
        x * lax.rsqrt(jnp.mean(x * x, axis=-1, keepdims=True) + NORM_EPS) * gain[...]
    ).astype(BF16)

    def project(index):
        copies[index].wait()
        return dot(normed, order[index][1][...]).astype(BF16).astype(F32)

    key_all = project(1)
    ones = jnp.where(head_blocks(width), 1.0, 0.0).astype(BF16)
    unit = key_all * kgain[...]
    unit = unit * lax.rsqrt(mm_left(unit * unit, ones) + KEY_EPS)
    erase = unit * jax.nn.sigmoid(project(2))
    copies[3].wait()
    copies[4].wait()
    logits = project(5) + bias[...] + shift[...]
    decay = jax.nn.sigmoid(logits) * (-0.6065306597126334) + extra[...]
    row, col = iota2(PAIR, PAIR)
    same = (row // CHUNK) == (col // CHUNK)
    strict = same & (row > col)
    inclusive = same & (row >= col)
    eye = jnp.where(row == col, 1.0, 0.0)
    tri = jnp.where(inclusive, 1.0, 0.0).astype(BF16)
    cum = jnp.concatenate(
        [mm_right(tri, decay[p * PAIR:(p + 1) * PAIR], count=3) for p in range(pairs)], axis=0
    )

    def chunk_row(offset):
        return jnp.concatenate(
            [
                jnp.broadcast_to(cum[c + offset:c + offset + 1], (CHUNK, width))
                for c in range(0, rows, CHUNK)
            ],
            axis=0,
        )

    mid = chunk_row(CHUNK // 2 - 1)
    final = chunk_row(CHUNK - 1)
    before = cum - decay
    up = jnp.exp(mid - cum)
    left_unit = unit * jnp.exp(before - mid)
    right_erase = erase * up
    right_key = key_all * up
    query_unit = unit * jnp.exp(before)
    keep = jnp.exp(final - cum)
    kept_erase = erase * keep
    kept_key = key_all * keep
    value = project(6)

    units = [(h, p) for h in range(heads) for p in range(pairs)]

    def piece(values, unit_index):
        h, p = unit_index
        return values[p * PAIR:(p + 1) * PAIR, h * HEAD:(h + 1) * HEAD]

    lower, key_mix, values_of, rights = [], [], [], []
    for u in units:
        right = jnp.concatenate([piece(right_erase, u), piece(right_key, u)], axis=0)
        product = mm(piece(left_unit, u), right, "qk", NT)
        lower.append(jnp.where(strict, product[:, :PAIR], 0.0))
        key_mix.append(jnp.where(strict, product[:, PAIR:], 0.0))
        values_of.append(piece(value, u))
        rights.append(right)
    right_side = [
        -jnp.concatenate([mm(k, v, "kmv"), piece(query_unit, u)], axis=1)
        for k, v, u in zip(key_mix, values_of, units)
    ]
    first = strict & ((row // 2) == (col // 2))
    inverse = [eye - jnp.where(first, low, 0.0) for low in lower]
    size = 2
    while size < CHUNK:
        level = ((row // (2 * size)) == (col // (2 * size))) & ((row // size) > (col // size))
        inner = [mm(jnp.where(level, low, 0.0), inv, "inv") for low, inv in zip(lower, inverse)]
        inverse = [inv - mm(inv, step, "inv") for inv, step in zip(inverse, inner)]
        size *= 2
    removed = [mm(inv, rhs, "rem") for inv, rhs in zip(inverse, right_side)]
    if REFINE:
        left_over = [
            rhs - rem - mm(low, rem, "res") for rhs, rem, low in zip(right_side, removed, lower)
        ]
        removed = [
            rem + mm(inv, rest, "fix") for rem, inv, rest in zip(removed, inverse, left_over)
        ]
    eye_head = iota2(HEAD, HEAD)
    eye_head = eye_head[0] == eye_head[1]
    blocks = {}
    for h in range(heads):
        for p in range(pairs):
            index = h * pairs + p
            ke, kk = piece(kept_erase, (h, p)), piece(kept_key, (h, p))
            for half in range(PAIR // CHUNK):
                span = slice(half * CHUNK, (half + 1) * CHUNK)
                start = p * PAIR + half * CHUNK
                from_removed = mm(removed[index][span], ke[span], "keep", TN)
                base = from_removed[:HEAD] + mm(values_of[index][span], kk[span], "keep", TN)
                last = jnp.exp(final[start:start + 1, h * HEAD:(h + 1) * HEAD])
                trans = from_removed[HEAD:] + jnp.where(eye_head, last, 0.0)
                blocks[h, start // CHUNK] = (base, trans)
    priors = {}
    totals = [None] * heads
    for chunk in range(rows // CHUNK):
        for h in range(heads):
            base, trans = blocks[h, chunk]
            priors[h, chunk] = totals[h]
            if totals[h] is None:
                totals[h] = jnp.concatenate([base, trans], axis=0)
            else:
                moved = mm(totals[h], trans, "state")
                totals[h] = jnp.concatenate([moved[:HEAD] + base, moved[HEAD:]], axis=0)
    own_total = jnp.concatenate(totals, axis=1).astype(WIRE)
    own_map[...] = own_total

    pl.semaphore_wait(barrier, n_sp + n_tp - 2)
    pair_copy = pltpu.make_async_remote_copy(
        src_ref=own_map, dst_ref=partner_map, send_sem=pair_sem.at[0], recv_sem=pair_sem.at[1],
        device_id=(sp + 1 - 2 * parity, tp), device_id_type=MESH,
    )
    pair_copy.start()

    conv_value = project(7)
    conv_rows = (conv_value * jax.nn.sigmoid(project(8))).astype(BF16)
    conv_in[...] = conv_rows
    halo_copy = pltpu.make_async_remote_copy(
        src_ref=conv_in.at[pl.ds(rows - halo_rows, halo_rows)], dst_ref=halo,
        send_sem=halo_sem.at[0], recv_sem=halo_sem.at[1],
        device_id=(sp + 1, tp), device_id_type=MESH,
    )
    has_next = sp + 1 < n_sp

    @pl.when(has_next)
    def _():
        halo_copy.start()

    extended[halo_rows:, :] = conv_rows.astype(F32)

    def chain(carry, block):
        trans = block_diagonal(block[HEAD:], width)
        return mm(carry, trans, "enter")

    receptance = project(9)
    left_read = receptance * jnp.exp(cum - mid)
    query_read = receptance * jnp.exp(cum)

    pair_copy.wait()
    mine, theirs = own_total.astype(F32), partner_map[...].astype(F32)
    early = jnp.where(first_member, mine, theirs)
    late = jnp.where(first_member, theirs, mine)
    joined = chain(early, late)
    pair_map[:HEAD] = (joined[:HEAD] + late[:HEAD]).astype(WIRE)
    pair_map[HEAD:] = joined[HEAD:].astype(WIRE)

    def map_copy(ahead):
        return pltpu.make_async_remote_copy(
            src_ref=pair_map, dst_ref=maps.at[ahead],
            send_sem=map_send.at[ahead], recv_sem=map_recv.at[ahead],
            device_id=(sp + 2 * ahead, tp), device_id_type=MESH,
        )

    for ahead in range(1, groups):
        @pl.when(group + ahead < groups)
        def _():
            map_copy(ahead).start()

    @pl.when(sp > 0)
    def _():
        halo_copy.wait_recv()
        extended[:halo_rows, :] = halo[...].astype(F32)

    @pl.when(sp == 0)
    def _():
        extended[:halo_rows, :] = jnp.zeros((halo_rows, channels), F32)

    tap_count = taps.shape[0]
    total = jnp.zeros((rows, channels), F32)
    for offset in range(tap_count):
        begin = halo_rows - tap_count + 1 + offset
        total = total + taps[offset:offset + 1, :] * extended[begin:begin + rows, :]
    means = jnp.where(head_blocks(channels), 1.0 / HEAD, 0.0).astype(BF16)
    centred = total - mm_left(total, means)
    scaled = centred * lax.rsqrt(mm_left(centred * centred, means) + GROUP_EPS)
    conv_out[...] = jax.nn.silu(scaled * ggain[...] + gshift[...]).astype(BF16)

    span = rows // n_tp

    def spread(source, slots, send, recv):
        started = []
        for step in range(1, n_tp):
            target = lax.rem(tp + step, n_tp)
            begin = pl.multiple_of(target * span, span)
            copy = pltpu.make_async_remote_copy(
                src_ref=source.at[pl.ds(begin, span)], dst_ref=slots.at[step],
                send_sem=send.at[step], recv_sem=recv.at[step],
                device_id=(sp, target), device_id_type=MESH,
            )
            copy.start()
            started.append(copy)
        return started

    conv_copies = spread(conv_out, conv_slots, conv_send, conv_recv)

    zeros = jnp.zeros((PAIR, HEAD), F32)
    for index, u in enumerate(units):
        h, p = u
        product = mm(piece(left_read, u), rights[index], "qk", NT)
        mix = jnp.concatenate(
            [
                jnp.where(inclusive, product[:, :PAIR], 0.0),
                jnp.where(inclusive, product[:, PAIR:], 0.0),
            ],
            axis=1,
        )
        stacked = jnp.concatenate(
            [removed[index], jnp.concatenate([values_of[index], zeros], axis=1)], axis=0
        )
        readout = mm(mix, stacked, "read") + jnp.concatenate(
            [zeros, piece(query_read, u)], axis=1
        )
        for half in range(PAIR // CHUNK):
            start = p * PAIR + half * CHUNK
            lanes = slice(h * HEAD, (h + 1) * HEAD)
            read = readout[half * CHUNK:(half + 1) * CHUNK]
            prior = priors[h, start // CHUNK]
            if prior is not None:
                read = jnp.concatenate(
                    [read[:, :HEAD], jnp.zeros((CHUNK, HEAD), F32)], axis=1
                ) + mm(read[:, HEAD:], prior, "carry", NT)
            local_read[start:start + CHUNK, lanes] = read[:, :HEAD]
            carried[start:start + CHUNK, lanes] = read[:, HEAD:]
    gate = jax.nn.sigmoid(project(10)) * hgain[...]

    own = pl.multiple_of(tp * span, span)

    def gather(result, source, slots, arriving, weight, depth):
        result = result + dot(
            source[pl.ds(own, span)], weight[pl.ds(pl.multiple_of(tp * depth, depth), depth)]
        )
        for step in range(1, n_tp):
            arriving[step - 1].wait_recv()
            begin = lax.rem(tp - step + n_tp, n_tp) * depth
            result = result + dot(
                slots[step], weight[pl.ds(pl.multiple_of(begin, depth), depth)]
            )
        return result

    copies[11].wait()
    result = gather(
        jnp.zeros(out.shape, F32), conv_out, conv_slots, conv_copies, co_buf, channels
    )

    state[...] = jnp.zeros_like(state)
    for ahead in range(groups - 1, 0, -1):
        @pl.when(group >= ahead)
        def _():
            map_copy(ahead).wait_recv()
            block = maps[ahead].astype(F32)
            state[...] = chain(state[...], block) + block[:HEAD]

    behind = chain(state[...], early) + early[:HEAD]
    entering = jnp.where(first_member, state[...], behind)
    readout = local_read[...] + mm(carried[...], block_diagonal(entering, width), "enter", NT)
    head_means = jnp.where(head_blocks(width), 1.0 / HEAD, 0.0).astype(BF16)
    centred = readout - mm_left(readout, head_means)
    scaled = centred * lax.rsqrt(mm_left(centred * centred, head_means) + HEAD_EPS)
    mix_out[...] = (scaled * gate).astype(BF16)
    mix_copies = spread(mix_out, mix_slots, mix_send, mix_recv)
    copies[12].wait()
    result = gather(result, mix_out, mix_slots, mix_copies, ao_buf, width)
    out[...] = result.astype(BF16)
    for copy in conv_copies + mix_copies:
        copy.wait_send()

    @pl.when(has_next)
    def _():
        halo_copy.wait_send()

    for ahead in range(1, groups):
        @pl.when(group + ahead < groups)
        def _():
            map_copy(ahead).wait_send()


def local(
    n_sp, n_tp,
    tokens, input_norm_gain, convolution_value_weight, convolution_gate_weight,
    depthwise_taps_weight, convolution_group_gain, convolution_group_shift,
    receptance_weight, key_weight, value_weight, decay_weight, correction_rate_weight,
    output_gate_weight, key_prenorm_gain, decay_offset_bias, position_decay_shift,
    extra_log_decay, head_norm_gain, convolution_output_weight, attention_output_weight,
):
    rows, model = tokens.shape
    channels = convolution_value_weight.shape[1]
    width = key_weight.shape[1]
    vmem = pl.BlockSpec(memory_space=pltpu.VMEM)
    anywhere = pl.BlockSpec(memory_space=pl.ANY)

    def line(values):
        return values.reshape(1, -1)

    weights = (
        convolution_value_weight, convolution_gate_weight, key_weight, receptance_weight,
        decay_weight, correction_rate_weight, value_weight, output_gate_weight,
        convolution_output_weight, attention_output_weight,
    )
    span = rows // n_tp
    halo_rows = -(-(depthwise_taps_weight.shape[0] - 1) // 16) * 16
    groups = n_sp // 2
    dma = pltpu.SemaphoreType.DMA
    map_shape = (2 * HEAD, width)
    return pl.pallas_call(
        functools.partial(layer_kernel, n_sp, n_tp),
        name="layer",
        out_shape=jax.ShapeDtypeStruct((span, model), BF16),
        in_specs=[vmem] * 7 + [anywhere] * 13,
        out_specs=vmem,
        scratch_shapes=[
            pltpu.VMEM(tokens.shape, BF16),
            pltpu.VMEM(position_decay_shift.shape, F32),
            pltpu.VMEM(extra_log_decay.shape, F32),
        ]
        + [pltpu.VMEM(weight.shape, BF16) for weight in weights]
        + [
            pltpu.VMEM((rows, channels), BF16),
            pltpu.VMEM((halo_rows + rows, channels), F32),
            pltpu.VMEM((halo_rows, channels), BF16),
            pltpu.VMEM(map_shape, WIRE),
            pltpu.VMEM(map_shape, WIRE),
            pltpu.VMEM(map_shape, WIRE),
            pltpu.VMEM((groups,) + map_shape, WIRE),
            pltpu.VMEM((HEAD, width), F32),
            pltpu.VMEM((rows, width), F32),
            pltpu.VMEM((rows, width), F32),
            pltpu.VMEM((rows, channels), BF16),
            pltpu.VMEM((rows, width), BF16),
            pltpu.VMEM((n_tp, span, channels), BF16),
            pltpu.VMEM((n_tp, span, width), BF16),
            dma((13,)), dma((2,)), dma((2,)), dma((groups,)), dma((groups,)),
            dma((n_tp,)), dma((n_tp,)), dma((n_tp,)), dma((n_tp,)),
        ],
        compiler_params=pltpu.CompilerParams(
            collective_id=0, has_side_effects=True, vmem_limit_bytes=VMEM_LIMIT
        ),
    )(
        line(input_norm_gain), line(key_prenorm_gain), line(decay_offset_bias),
        depthwise_taps_weight, line(convolution_group_gain), line(convolution_group_shift),
        line(head_norm_gain), tokens, position_decay_shift, extra_log_decay, *weights,
    )


def solution(mesh):
    in_specs = (
        P("sp", None),
        P(),
        P(None, "tp"),
        P(None, "tp"),
        P(None, "tp"),
        P("tp"),
        P("tp"),
        P(None, "tp"),
        P(None, "tp"),
        P(None, "tp"),
        P(None, "tp"),
        P(None, "tp"),
        P(None, "tp"),
        P("tp"),
        P("tp"),
        P("sp", "tp"),
        P("sp", "tp"),
        P("tp"),
        P(),
        P(),
    )
    body = functools.partial(local, mesh.shape["sp"], mesh.shape["tp"])
    return jax.shard_map(
        body, mesh=mesh, in_specs=in_specs, out_specs=P(("sp", "tp"), None), check_vma=False
    )
```
